32 devices in a mesh: sp: 16 (over z, y, core), tp: 2 (over x).
Axes of the slice: x: 2, y: 2, z: 4, core: 2. Of those that a mesh axis runs over, the one named last changes fastest.
Arguments:
- queries: bfloat16 [16384, 1024], P('sp', 'tp'), may hold values from -8 to 8
- keys: bfloat16 [16384, 256], P('sp', 'tp'), may hold values from -8 to 8
- values: bfloat16 [16384, 256], P('sp', 'tp'), may hold values from -18 to 18
- doc_ids: int32 [16384], P('sp'), may hold values from 0 to 3, never falling along the last dimension, each value on 1 to 8192 neighbouring positions
- sinks: float32 [16], P('tp'), may hold values from 0 to 4
- residual: bfloat16 [16384, 2048], P(('sp', 'tp')), may hold values from -12 to 12
- out_weight: bfloat16 [1024, 2048], P('tp'), may hold values from -0.1875 to 0.1875
- norm_gain: float32 [2048], replicated, may hold values from 0.1 to 1.9
- w_gate: bfloat16 [2048, 5632], P('sp', 'tp'), may hold values from -0.125 to 0.125
- w_value: bfloat16 [2048, 5632], P('sp', 'tp'), may hold values from -0.125 to 0.125
- conv_gate: float32 [3, 5632], P(None, 'tp'), may hold values from -3.5 to 3.5
- conv_value: float32 [3, 5632], P(None, 'tp'), may hold values from -3.5 to 3.5
- w_down: bfloat16 [5632, 2048], P('tp', 'sp'), may hold values from -0.078125 to 0.078125
Outputs:
- layer_out: bfloat16 [16384, 2048], P(('sp', 'tp'))
The draws below stay inside these ranges and needn't reach their ends.
All inputs are finite; a program needn't handle non-finite values.
Results may differ from the reference program's by a relative error of at most 0.012.
Values may be sent and summed in bfloat16 or wider, within the bound.
A program may use at most 128 MiB of HBM per device.

```python
import math
import jax
import jax.numpy as jnp
import numpy as np
from jax import lax

D = 2048
HEAD_DIM = 64
A_HEADS = 16
FF = 5632
WINDOW = 128
TOK_SP = 1024
TOKENS = 16384
A_Q = 1024
KV_W = 256
DOCS = 4
N_SP = 16


def draw_keys(key, part):
    base = jnp.clip(jax.random.normal(jax.random.fold_in(key, 1), (TOKENS, KV_W), jnp.float32), -8.0, 8.0)
    return base.astype(jnp.bfloat16)


def draw_queries(key, part):
    base = jnp.clip(jax.random.normal(jax.random.fold_in(key, 2), (TOKENS, A_Q), jnp.float32), -8.0, 8.0)
    return base.astype(jnp.bfloat16)


def draw_residual(key, part):
    base = jax.random.normal(jax.random.fold_in(key, 3), (TOKENS, D), jnp.float32)
    spread = jax.random.uniform(jax.random.fold_in(key, 4), (TOKENS, 1), jnp.float32, math.log(1.0 / 3.0), math.log(3.0))
    base = base * jnp.exp(spread)
    return jnp.clip(base, -12.0, 12.0).astype(jnp.bfloat16)


def shard_levels(key, shape, shards, least, top_value):
    gain, own = 1.0, jax.random.fold_in(key, 6)
    for dim, shards_of in shards:
        heights = jnp.exp(jax.random.uniform(jax.random.fold_in(own, dim), (shards_of,), jnp.float32, least / len(shards), top_value / len(shards)))
        gain = gain * jnp.repeat(heights, shape[dim] // shards_of).reshape([-1 if axis == dim else 1 for axis in range(len(shape))])
    return gain


def split_up(number_of, total, most, slope):
    portions = [(1 << 20) // math.isqrt(grade ** slope) + 1 for grade in range(2, number_of + 1)]
    rest, counts = total - most - (number_of - 1), [1] * (number_of - 1)
    while rest > 0:
        movable = [i for i in range(number_of - 1) if counts[i] < most]
        whole, left = sum([portions[i] for i in movable]), rest
        for i in movable:
            addition = min(most - counts[i], max(1, left * portions[i] // whole), rest)
            counts[i] = counts[i] + addition
            rest = rest - addition
    return np.array([most] + counts)


def ragged(stream_key, count, total, reach, slope):
    if count == 2:
        one = jax.random.randint(stream_key, (), max(1, total - reach), min(reach, total - 1) + 1)
        return jnp.stack([one, total - one])
    tallies = jnp.asarray(split_up(count, total, reach, slope), jnp.int32)
    couples = (count - 1) // 2
    donor, receiver = tallies[1:1 + 2 * couples:2], tallies[2:2 + 2 * couples:2]
    slack = jnp.minimum(donor - 1, reach - receiver)
    shifted = jax.random.randint(jax.random.fold_in(stream_key, 1), (couples,), 0, 1 << 20) % (slack + 1)
    tallies = tallies.at[1:1 + 2 * couples:2].set(donor - shifted).at[2:2 + 2 * couples:2].set(receiver + shifted)
    return tallies[jax.random.permutation(jax.random.fold_in(stream_key, 2), count)]


def bell_draw(stream_key, shape, deviation, limit, cuts=(), held_as=jnp.bfloat16):
    entries = deviation * jax.random.normal(stream_key, shape, jnp.float32)
    if cuts:
        entries = entries * shard_levels(stream_key, shape, cuts, -0.22, 0.18)
    return jnp.clip(entries, -limit, limit).astype(held_as)


def setup_inputs(seed: int = 0) -> dict:
    streams_of = jax.random.split(jax.random.key(seed), 14)
    queries = draw_queries(jax.random.fold_in(streams_of[13], 71), 0)
    keys = draw_keys(jax.random.fold_in(streams_of[13], 71), 0)
    values = bell_draw(streams_of[2], (TOKENS, KV_W), 3.0, 18.0, ((0, 16), (1, 2)))
    doc_ids = jnp.searchsorted(jnp.cumsum(ragged(streams_of[3], DOCS, TOKENS, TOKENS // 2, 0)), jnp.arange(TOKENS), side="right").astype(jnp.int32)
    sinks = jnp.clip(4.0 * jax.random.uniform(streams_of[4], (A_HEADS,), jnp.float32) ** shard_levels(streams_of[4], (A_HEADS,), ((0, 2),), -0.2, 0.2), 0.0, 4.0)
    residual = draw_residual(jax.random.fold_in(streams_of[13], 71), 0)
    out_weight = bell_draw(streams_of[6], (A_Q, D), A_Q ** -0.5, 0.1875, ((0, 2),))
    norm_gain = jnp.clip(1.0 + 0.18 * jax.random.normal(streams_of[7], (D,), jnp.float32), 0.1, 1.9)
    w_gate = bell_draw(streams_of[8], (D, FF), D ** -0.5, 0.125, ((0, 16), (1, 2)))
    w_value = bell_draw(streams_of[9], (D, FF), D ** -0.5, 0.125, ((0, 16), (1, 2)))
    conv_gate = bell_draw(streams_of[10], (3, FF), 3 ** -0.5, 3.5, ((1, 2),), jnp.float32)
    conv_value = bell_draw(streams_of[11], (3, FF), 3 ** -0.5, 3.5, ((1, 2),), jnp.float32)
    w_down = bell_draw(streams_of[12], (FF, D), FF ** -0.5, 0.078125, ((0, 2), (1, 16)))
    return dict(queries=queries, keys=keys, values=values, doc_ids=doc_ids, sinks=sinks, residual=residual, out_weight=out_weight, norm_gain=norm_gain, w_gate=w_gate, w_value=w_value, conv_gate=conv_gate, conv_value=conv_value, w_down=w_down)


def attend(query_rows, key_ext, value_ext, doc_rows, doc_ext, sinks):
    row_count = query_rows.shape[0]
    block_count = row_count // WINDOW
    kv_heads = key_ext.shape[1] // HEAD_DIM
    group_size = query_rows.shape[1] // (kv_heads * HEAD_DIM)

    def band(t):
        lower = t[:row_count].reshape((block_count, WINDOW) + t.shape[1:])
        upper = t[WINDOW:].reshape((block_count, WINDOW) + t.shape[1:])
        return jnp.concatenate([lower, upper], axis=1)
    query_band = query_rows.astype(jnp.float32).reshape(block_count, WINDOW, kv_heads, group_size, HEAD_DIM)
    key_band = band(key_ext).astype(jnp.float32).reshape(block_count, 2 * WINDOW, kv_heads, HEAD_DIM)
    value_band = band(value_ext).astype(jnp.float32).reshape(block_count, 2 * WINDOW, kv_heads, HEAD_DIM)
    doc_band = band(doc_ext)
    distance = jnp.arange(WINDOW)[:, None] + WINDOW - jnp.arange(2 * WINDOW)[None, :]
    in_window = (distance >= 0) & (distance < WINDOW)
    same_doc = doc_rows.reshape(block_count, WINDOW)[:, :, None] == doc_band[:, None, :]
    keep_mask = in_window[None] & same_doc
    scores = jnp.einsum('nqhgd,nkhd->nhgqk', query_band, key_band) * HEAD_DIM ** (-0.5)
    scores = jnp.where(keep_mask[:, None, None], scores, -jnp.inf)
    sink_logit = sinks.astype(jnp.float32).reshape(kv_heads, group_size)[None, :, :, None, None]
    peak = jnp.maximum(lax.optimization_barrier(jnp.max(scores, axis=-1, keepdims=True)), sink_logit)
    expd = jnp.exp(scores - peak)
    probs = (expd / (lax.optimization_barrier(jnp.sum(expd, axis=-1, keepdims=True)) + jnp.exp(sink_logit - peak))).astype(jnp.bfloat16)
    mixed = jnp.einsum('nhgqk,nkhd->nqhgd', probs.astype(jnp.float32), value_band)
    return mixed.astype(jnp.bfloat16).reshape(row_count, -1)

def convolve(ext_rows, doc_ext, taps):
    center = doc_ext[2:]
    same_one = (doc_ext[1:-1] == center)[:, None]
    same_two = (doc_ext[:-2] == center)[:, None]
    ext32 = ext_rows.astype(jnp.float32)
    result = taps[2] * ext32[2:]
    result = result + jnp.where(same_one, taps[1] * ext32[1:-1], 0.0)
    return result + jnp.where(same_two, taps[0] * ext32[:-2], 0.0)

def reference(queries, keys, values, doc_ids, sinks, residual, out_weight, norm_gain, w_gate, w_value, conv_gate, conv_value, w_down):
    docs_plus = doc_ids + 1
    key_pad = jnp.concatenate([jnp.zeros((WINDOW, KV_W), jnp.bfloat16), keys], axis=0)
    value_pad = jnp.concatenate([jnp.zeros((WINDOW, KV_W), jnp.bfloat16), values], axis=0)
    doc_pad = jnp.concatenate([jnp.zeros((WINDOW,), jnp.int32), docs_plus], axis=0)

    def attend_shard(index):
        start = (index * TOK_SP).astype(jnp.int32)
        return attend(lax.dynamic_slice_in_dim(queries, start, TOK_SP, 0), lax.dynamic_slice_in_dim(key_pad, start, TOK_SP + WINDOW, 0), lax.dynamic_slice_in_dim(value_pad, start, TOK_SP + WINDOW, 0), lax.dynamic_slice_in_dim(docs_plus, start, TOK_SP, 0), lax.dynamic_slice_in_dim(doc_pad, start, TOK_SP + WINDOW, 0), sinks)
    shard_ids = jnp.arange(N_SP, dtype=jnp.int32)
    attn = lax.map(attend_shard, shard_ids).reshape(TOKENS, A_Q)
    proj = jnp.dot(attn, out_weight, preferred_element_type=jnp.float32)
    mid = (residual.astype(jnp.float32) + proj).astype(jnp.bfloat16)
    mid32 = mid.astype(jnp.float32)
    normed = (mid32 * lax.rsqrt(lax.optimization_barrier(jnp.mean(mid32 * mid32, axis=-1, keepdims=True)) + 1e-06) * norm_gain).astype(jnp.bfloat16)
    normed_pad = jnp.concatenate([jnp.zeros((2, D), jnp.bfloat16), normed], axis=0)
    doc_two = jnp.concatenate([jnp.zeros((2,), jnp.int32), docs_plus], axis=0)

    def mlp_shard(index):
        start = (index * TOK_SP).astype(jnp.int32)
        rows_ext = lax.dynamic_slice_in_dim(normed_pad, start, TOK_SP + 2, 0)
        doc_ext = lax.dynamic_slice_in_dim(doc_two, start, TOK_SP + 2, 0)
        gate_pre = jnp.dot(rows_ext, w_gate, preferred_element_type=jnp.float32).astype(jnp.bfloat16)
        value_pre = jnp.dot(rows_ext, w_value, preferred_element_type=jnp.float32).astype(jnp.bfloat16)
        gate_conv = convolve(gate_pre, doc_ext, conv_gate)
        value_conv = convolve(value_pre, doc_ext, conv_value)
        hidden = (jax.nn.silu(gate_conv) * value_conv).astype(jnp.bfloat16)
        return jnp.dot(hidden, w_down, preferred_element_type=jnp.float32)
    mlp = lax.map(mlp_shard, shard_ids).reshape(TOKENS, D)
    return (mid32 + mlp).astype(jnp.bfloat16)
```

```python
import jax
import jax.numpy as jnp
from jax import lax
from jax.experimental import pallas as pl
from jax.sharding import PartitionSpec as P


HEAD_DIM = 64
WINDOW = 128
ROW_TILE = 128


def shifted(shard, axis, by):
    size = lax.axis_size(axis)
    pairs = [(i, i + by) for i in range(size) if 0 <= i + by < size]
    return lax.ppermute(shard, axis, pairs)


def turned(t, axis, by):
    size = lax.axis_size(axis)
    return lax.ppermute(t, axis, [(i, (i + by) % size) for i in range(size)])


def core_swap(t):
    size = lax.axis_size("sp")
    return lax.ppermute(t, "sp", [(i, i ^ 1) for i in range(size)])


def parity_gather(t):
    size = lax.axis_size("sp")
    groups = [list(range(0, size, 2)), list(range(1, size, 2))]
    return lax.all_gather(t, "sp", axis=0, tiled=True, axis_index_groups=groups)


def by_parity(t, depth):
    rows, width = t.shape
    blocks = width // depth
    tile = min(ROW_TILE, rows)

    def kernel(in_ref, out_ref):
        for j in range(blocks):
            to = (j // 2 + (j % 2) * (blocks // 2)) * depth
            out_ref[:, to : to + depth] = in_ref[:, j * depth : (j + 1) * depth]

    return pl.pallas_call(
        kernel,
        out_shape=jax.ShapeDtypeStruct(t.shape, t.dtype),
        grid=(rows // tile,),
        in_specs=[pl.BlockSpec((tile, width), lambda i: (i, 0))],
        out_specs=pl.BlockSpec((tile, width), lambda i: (i, 0)),
        cost_estimate=pl.CostEstimate(
            flops=0, bytes_accessed=2 * t.size * t.dtype.itemsize, transcendentals=0
        ),
    )(t)


def finish(mid, sums, depth):
    rows, width = mid.shape
    blocks = width // depth
    tile = min(ROW_TILE, rows)

    def kernel(mid_ref, even_ref, odd_ref, out_ref):
        for j in range(blocks):
            at = (j // 2) * depth
            held = at + (j % 2) * (width // 2)
            sum_ref = odd_ref if j % 2 else even_ref
            out_ref[:, j * depth : (j + 1) * depth] = (
                mid_ref[:, held : held + depth].astype(jnp.float32)
                + sum_ref[:, at : at + depth]
            ).astype(out_ref.dtype)

    half_spec = pl.BlockSpec((tile, width // 2), lambda i: (i, 0))
    return pl.pallas_call(
        kernel,
        out_shape=jax.ShapeDtypeStruct(mid.shape, mid.dtype),
        grid=(rows // tile,),
        in_specs=[pl.BlockSpec((tile, width), lambda i: (i, 0)), half_spec, half_spec],
        out_specs=pl.BlockSpec((tile, width), lambda i: (i, 0)),
        cost_estimate=pl.CostEstimate(
            flops=mid.size, bytes_accessed=8 * mid.size, transcendentals=0
        ),
    )(mid, *sums)


def attend(query_rows, key_ext, value_ext, doc_rows, doc_ext, sinks):
    row_count = query_rows.shape[0]
    block_count = row_count // WINDOW
    kv_heads = key_ext.shape[1] // HEAD_DIM
    group_size = query_rows.shape[1] // (kv_heads * HEAD_DIM)

    def band(t):
        lower = t[:row_count].reshape((block_count, WINDOW) + t.shape[1:])
        upper = t[WINDOW:].reshape((block_count, WINDOW) + t.shape[1:])
        return jnp.concatenate([lower, upper], axis=1)

    query_band = query_rows.reshape(block_count, WINDOW, kv_heads, group_size, HEAD_DIM)
    key_band = band(key_ext).reshape(block_count, 2 * WINDOW, kv_heads, HEAD_DIM)
    value_band = band(value_ext).reshape(block_count, 2 * WINDOW, kv_heads, HEAD_DIM)
    doc_band = band(doc_ext)
    distance = jnp.arange(WINDOW)[:, None] + WINDOW - jnp.arange(2 * WINDOW)[None, :]
    in_window = (distance >= 0) & (distance < WINDOW)
    same_doc = doc_rows.reshape(block_count, WINDOW)[:, :, None] == doc_band[:, None, :]
    keep_mask = in_window[None] & same_doc
    scores = jnp.einsum(
        "nqhgd,nkhd->nhgqk", query_band, key_band, preferred_element_type=jnp.float32
    ) * HEAD_DIM ** (-0.5)
    scores = jnp.where(keep_mask[:, None, None], scores, -jnp.inf)
    sink_logit = sinks.reshape(kv_heads, group_size)[None, :, :, None, None]
    peak = jnp.maximum(jnp.max(scores, axis=-1, keepdims=True), sink_logit)
    expd = jnp.exp(scores - peak)
    probs = (expd / (jnp.sum(expd, axis=-1, keepdims=True) + jnp.exp(sink_logit - peak))).astype(
        jnp.bfloat16
    )
    mixed = jnp.einsum("nhgqk,nkhd->nqhgd", probs, value_band, preferred_element_type=jnp.float32)
    return mixed.astype(jnp.bfloat16).reshape(row_count, -1)


def convolve(ext_rows, doc_ext, taps):
    center = doc_ext[2:]
    same_one = (doc_ext[1:-1] == center)[:, None]
    same_two = (doc_ext[:-2] == center)[:, None]
    ext32 = ext_rows.astype(jnp.float32)
    result = taps[2] * ext32[2:]
    result = result + jnp.where(same_one, taps[1] * ext32[1:-1], 0.0)
    return result + jnp.where(same_two, taps[0] * ext32[:-2], 0.0)


def per_device(
    queries,
    keys,
    values,
    doc_ids,
    sinks,
    residual,
    out_weight,
    norm_gain,
    w_gate,
    w_value,
    conv_gate,
    conv_value,
    w_down,
):
    core = lax.axis_index("sp") % 2
    tp = lax.axis_index("tp")
    n_tp = lax.axis_size("tp")
    rows = doc_ids.shape[0]
    part_rows = rows // n_tp
    depth = w_gate.shape[0]
    width = residual.shape[1]
    half = width // 2
    part_index = [(tp + n_tp - d) % n_tp for d in range(n_tp)]

    gate_own = parity_gather(w_gate)
    value_own = parity_gather(w_value)
    down_t = w_down.T
    inner = down_t.shape[1] // 2
    low, high = down_t[:, :inner], down_t[:, inner:]
    kept_half = jnp.where(core == 0, low, high)
    came_half = core_swap(jnp.where(core == 0, high, low))
    even_piece = jnp.where(core == 0, kept_half, came_half)
    odd_piece = jnp.where(core == 0, came_half, kept_half)
    down_odd = parity_gather(odd_piece)
    down_even = parity_gather(even_piece)
    gate_far = core_swap(gate_own)
    value_far = core_swap(value_own)

    out_far = [turned(out_weight, "tp", d) for d in range(1, n_tp)]
    out_parts = [by_parity(t, depth) for t in [out_weight] + out_far]
    residual = by_parity(residual, depth)
    norm_gain = norm_gain.reshape(-1, 2, depth).swapaxes(0, 1).reshape(-1)
    docs_plus = doc_ids + 1
    prev_keys, prev_values, prev_docs = shifted(
        (keys[-WINDOW:], values[-WINDOW:], docs_plus[-WINDOW:]), "sp", 1
    )
    key_ext = jnp.concatenate([prev_keys, keys], axis=0)
    value_ext = jnp.concatenate([prev_values, values], axis=0)
    doc_ext = jnp.concatenate([prev_docs, docs_plus], axis=0)
    head_out = attend(queries, key_ext, value_ext, docs_plus, doc_ext, sinks)

    def rows_of(t, index):
        return lax.dynamic_slice_in_dim(t, index * part_rows, part_rows, 0)

    proj = jnp.dot(rows_of(head_out, tp), out_parts[0], preferred_element_type=jnp.float32)
    for d in range(1, n_tp):
        heads_far = turned(rows_of(head_out, (tp + d) % n_tp), "tp", d)
        proj = proj + jnp.dot(heads_far, out_parts[d], preferred_element_type=jnp.float32)
    mid = (residual.astype(jnp.float32) + proj).astype(jnp.bfloat16)
    mid32 = mid.astype(jnp.float32)
    normed = (
        mid32 * lax.rsqrt(jnp.mean(mid32 * mid32, axis=-1, keepdims=True) + 1e-06) * norm_gain
    ).astype(jnp.bfloat16)
    even, odd = normed[:, :half], normed[:, half:]
    own = [jnp.where(core == 0, even, odd)]
    far = [jnp.where(core == 0, odd, even)]
    for d in range(1, n_tp):
        own.append(turned(own[0], "tp", d))
        far.append(turned(far[0], "tp", d))

    def up(own, far, w_own, w_far):
        total = jnp.dot(own, w_own, preferred_element_type=jnp.float32)
        return (total + jnp.dot(far, w_far, preferred_element_type=jnp.float32)).astype(
            jnp.bfloat16
        )

    gate_parts = [up(o, f, gate_own, gate_far) for o, f in zip(own, far)]
    value_parts = [up(o, f, value_own, value_far) for o, f in zip(own, far)]

    conv_docs = jnp.concatenate([prev_docs[-2:], docs_plus], axis=0)
    part_docs = [
        lax.dynamic_slice_in_dim(conv_docs, i * part_rows, part_rows + 2, 0) for i in part_index
    ]

    def conv_parts(parts, taps):
        tails = [p[-2:] for p in parts]
        last = tails[0]
        for d in range(1, n_tp):
            last = jnp.where(part_index[d] == n_tp - 1, tails[d], last)
        prev = shifted(last, "sp", 1)
        result = []
        for d in range(n_tp):
            halo = jnp.where(part_index[d] == 0, prev, tails[(d + 1) % n_tp])
            result.append(
                convolve(jnp.concatenate([halo, parts[d]], axis=0), part_docs[d], taps)
            )
        return result

    gate_conv = conv_parts(gate_parts, conv_gate)
    value_conv = conv_parts(value_parts, conv_value)
    hidden = [
        (jax.nn.silu(g) * v).astype(jnp.bfloat16) for g, v in zip(gate_conv, value_conv)
    ]

    def down(units, w_t):
        return lax.dot_general(
            units, w_t, (((1,), (1,)), ((), ())), preferred_element_type=jnp.float32
        )

    own_units = [jnp.where(core == 0, h[:, :inner], h[:, inner:]) for h in hidden]
    far_units = [jnp.where(core == 0, h[:, inner:], h[:, :inner]) for h in hidden]

    def down_sums(w_own):
        w_far = core_swap(w_own)
        came = []
        for d in range(1, n_tp):
            sent = (down(own_units[d], w_own) + down(far_units[d], w_far)).astype(
                jnp.bfloat16
            )
            came.append(turned(sent, "tp", -d))
        kept = down(own_units[0], w_own) + down(far_units[0], w_far)
        for t in came:
            kept = kept + t.astype(jnp.float32)
        return kept

    odd_sum = down_sums(down_odd)
    even_sum = down_sums(down_even)
    sums = (even_sum, odd_sum)
    return finish(mid, sums, depth)


def solution(mesh):
    return jax.shard_map(
        per_device,
        mesh=mesh,
        in_specs=(
            P("sp", "tp"),
            P("sp", "tp"),
            P("sp", "tp"),
            P("sp"),
            P("tp"),
            P(("sp", "tp"), None),
            P("tp", None),
            P(),
            P("sp", "tp"),
            P("sp", "tp"),
            P(None, "tp"),
            P(None, "tp"),
            P("tp", "sp"),
        ),
        out_specs=P(("sp", "tp"), None),
        check_vma=False,
    )
```

```python
import jax
import jax.numpy as jnp
from jax import lax
from jax.experimental import pallas as pl
from jax.sharding import PartitionSpec as P


HEAD_DIM = 64
WINDOW = 128
ROW_TILE = 128


def shifted(shard, axis, by):
    size = lax.axis_size(axis)
    pairs = [(i, i + by) for i in range(size) if 0 <= i + by < size]
    return lax.ppermute(shard, axis, pairs)


def turned(t, axis, by):
    size = lax.axis_size(axis)
    return lax.ppermute(t, axis, [(i, (i + by) % size) for i in range(size)])


def core_swap(t):
    size = lax.axis_size("sp")
    return lax.ppermute(t, "sp", [(i, i ^ 1) for i in range(size)])


def parity_gather(t):
    size = lax.axis_size("sp")
    groups = [list(range(0, size, 2)), list(range(1, size, 2))]
    return lax.all_gather(t, "sp", axis=0, tiled=True, axis_index_groups=groups)


def ring_gather(t):
    chips = lax.axis_size("sp") // 2
    order = list(range(0, chips, 2)) + list(range(1, chips, 2))[::-1]
    chip = lax.axis_index("sp") // 2
    place = jnp.where(chip % 2 == 0, chip // 2, chips - 1 - chip // 2)

    def hop(piece, by):
        pairs = [
            (2 * order[k] + c, 2 * order[(k + by) % chips] + c)
            for k in range(chips)
            for c in range(2)
        ]
        return lax.ppermute(piece, "sp", pairs)

    def chip_at(k):
        k = (k + chips) % chips
        return jnp.where(k < chips // 2, 2 * k, 2 * (chips - 1 - k) + 1)

    depth = t.shape[0]
    pieces = [(chip, t)]
    up = down = t
    for step in range(1, chips // 2 + 1):
        up = hop(up, 1)
        pieces.append((chip_at(place - step), up))
        if step < chips - step:
            down = hop(down, -1)
            pieces.append((chip_at(place + step), down))
    whole = jnp.zeros((chips * depth,) + t.shape[1:], t.dtype)
    for at, piece in pieces:
        whole = lax.dynamic_update_slice_in_dim(whole, piece, at * depth, 0)
    return whole


def by_parity(t, depth):
    rows, width = t.shape
    blocks = width // depth
    tile = min(ROW_TILE, rows)

    def kernel(in_ref, out_ref):
        for j in range(blocks):
            to = (j // 2 + (j % 2) * (blocks // 2)) * depth
            out_ref[:, to : to + depth] = in_ref[:, j * depth : (j + 1) * depth]

    return pl.pallas_call(
        kernel,
        out_shape=jax.ShapeDtypeStruct(t.shape, t.dtype),
        grid=(rows // tile,),
        in_specs=[pl.BlockSpec((tile, width), lambda i: (i, 0))],
        out_specs=pl.BlockSpec((tile, width), lambda i: (i, 0)),
        cost_estimate=pl.CostEstimate(
            flops=0, bytes_accessed=2 * t.size * t.dtype.itemsize, transcendentals=0
        ),
    )(t)


def finish(mid, sums, depth):
    rows, width = mid.shape
    blocks = width // depth
    tile = min(ROW_TILE, rows)

    def kernel(mid_ref, even_ref, odd_ref, out_ref):
        for j in range(blocks):
            at = (j // 2) * depth
            held = at + (j % 2) * (width // 2)
            sum_ref = odd_ref if j % 2 else even_ref
            out_ref[:, j * depth : (j + 1) * depth] = (
                mid_ref[:, held : held + depth].astype(jnp.float32)
                + sum_ref[:, at : at + depth]
            ).astype(out_ref.dtype)

    half_spec = pl.BlockSpec((tile, width // 2), lambda i: (i, 0))
    return pl.pallas_call(
        kernel,
        out_shape=jax.ShapeDtypeStruct(mid.shape, mid.dtype),
        grid=(rows // tile,),
        in_specs=[pl.BlockSpec((tile, width), lambda i: (i, 0)), half_spec, half_spec],
        out_specs=pl.BlockSpec((tile, width), lambda i: (i, 0)),
        cost_estimate=pl.CostEstimate(
            flops=mid.size, bytes_accessed=8 * mid.size, transcendentals=0
        ),
    )(mid, *sums)


def attend(query_rows, key_ext, value_ext, doc_rows, doc_ext, sinks):
    row_count = query_rows.shape[0]
    block_count = row_count // WINDOW
    kv_heads = key_ext.shape[1] // HEAD_DIM
    group_size = query_rows.shape[1] // (kv_heads * HEAD_DIM)

    def band(t):
        lower = t[:row_count].reshape((block_count, WINDOW) + t.shape[1:])
        upper = t[WINDOW:].reshape((block_count, WINDOW) + t.shape[1:])
        return jnp.concatenate([lower, upper], axis=1)

    query_band = query_rows.reshape(block_count, WINDOW, kv_heads, group_size, HEAD_DIM)
    key_band = band(key_ext).reshape(block_count, 2 * WINDOW, kv_heads, HEAD_DIM)
    value_band = band(value_ext).reshape(block_count, 2 * WINDOW, kv_heads, HEAD_DIM)
    doc_band = band(doc_ext)
    distance = jnp.arange(WINDOW)[:, None] + WINDOW - jnp.arange(2 * WINDOW)[None, :]
    in_window = (distance >= 0) & (distance < WINDOW)
    same_doc = doc_rows.reshape(block_count, WINDOW)[:, :, None] == doc_band[:, None, :]
    keep_mask = in_window[None] & same_doc
    scores = jnp.einsum(
        "nqhgd,nkhd->nhgqk", query_band, key_band, preferred_element_type=jnp.float32
    ) * HEAD_DIM ** (-0.5)
    scores = jnp.where(keep_mask[:, None, None], scores, -jnp.inf)
    sink_logit = sinks.reshape(kv_heads, group_size)[None, :, :, None, None]
    peak = jnp.maximum(jnp.max(scores, axis=-1, keepdims=True), sink_logit)
    expd = jnp.exp(scores - peak)
    probs = (expd / (jnp.sum(expd, axis=-1, keepdims=True) + jnp.exp(sink_logit - peak))).astype(
        jnp.bfloat16
    )
    mixed = jnp.einsum("nhgqk,nkhd->nqhgd", probs, value_band, preferred_element_type=jnp.float32)
    return mixed.astype(jnp.bfloat16).reshape(row_count, -1)


def convolve(ext_rows, doc_ext, taps):
    center = doc_ext[2:]
    same_one = (doc_ext[1:-1] == center)[:, None]
    same_two = (doc_ext[:-2] == center)[:, None]
    ext32 = ext_rows.astype(jnp.float32)
    result = taps[2] * ext32[2:]
    result = result + jnp.where(same_one, taps[1] * ext32[1:-1], 0.0)
    return result + jnp.where(same_two, taps[0] * ext32[:-2], 0.0)


def per_device(
    queries,
    keys,
    values,
    doc_ids,
    sinks,
    residual,
    out_weight,
    norm_gain,
    w_gate,
    w_value,
    conv_gate,
    conv_value,
    w_down,
):
    core = lax.axis_index("sp") % 2
    tp = lax.axis_index("tp")
    n_tp = lax.axis_size("tp")
    rows = doc_ids.shape[0]
    part_rows = rows // n_tp
    depth = w_gate.shape[0]
    width = residual.shape[1]
    half = width // 2
    part_index = [(tp + n_tp - d) % n_tp for d in range(n_tp)]

    gate_own = parity_gather(w_gate)
    value_own = ring_gather(w_value)
    down_t = w_down.T
    inner = down_t.shape[1] // 2
    low, high = down_t[:, :inner], down_t[:, inner:]
    kept_half = jnp.where(core == 0, low, high)
    came_half = core_swap(jnp.where(core == 0, high, low))
    even_piece = jnp.where(core == 0, kept_half, came_half)
    odd_piece = jnp.where(core == 0, came_half, kept_half)
    down_odd = parity_gather(odd_piece)
    down_even = parity_gather(even_piece)
    gate_far = core_swap(gate_own)
    value_far = core_swap(value_own)

    out_far = [turned(out_weight, "tp", d) for d in range(1, n_tp)]
    out_parts = [by_parity(t, depth) for t in [out_weight] + out_far]
    residual = by_parity(residual, depth)
    norm_gain = norm_gain.reshape(-1, 2, depth).swapaxes(0, 1).reshape(-1)
    docs_plus = doc_ids + 1
    prev_keys, prev_values, prev_docs = shifted(
        (keys[-WINDOW:], values[-WINDOW:], docs_plus[-WINDOW:]), "sp", 1
    )
    key_ext = jnp.concatenate([prev_keys, keys], axis=0)
    value_ext = jnp.concatenate([prev_values, values], axis=0)
    doc_ext = jnp.concatenate([prev_docs, docs_plus], axis=0)
    head_out = attend(queries, key_ext, value_ext, docs_plus, doc_ext, sinks)

    def rows_of(t, index):
        return lax.dynamic_slice_in_dim(t, index * part_rows, part_rows, 0)

    proj = jnp.dot(rows_of(head_out, tp), out_parts[0], preferred_element_type=jnp.float32)
    for d in range(1, n_tp):
        heads_far = turned(rows_of(head_out, (tp + d) % n_tp), "tp", d)
        proj = proj + jnp.dot(heads_far, out_parts[d], preferred_element_type=jnp.float32)
    mid = (residual.astype(jnp.float32) + proj).astype(jnp.bfloat16)
    mid32 = mid.astype(jnp.float32)
    normed = (
        mid32 * lax.rsqrt(jnp.mean(mid32 * mid32, axis=-1, keepdims=True) + 1e-06) * norm_gain
    ).astype(jnp.bfloat16)
    even, odd = normed[:, :half], normed[:, half:]
    own = [jnp.where(core == 0, even, odd)]
    far = [jnp.where(core == 0, odd, even)]
    for d in range(1, n_tp):
        own.append(turned(own[0], "tp", d))
        far.append(turned(far[0], "tp", d))

    def up(own, far, w_own, w_far):
        total = jnp.dot(own, w_own, preferred_element_type=jnp.float32)
        return (total + jnp.dot(far, w_far, preferred_element_type=jnp.float32)).astype(
            jnp.bfloat16
        )

    gate_parts = [up(o, f, gate_own, gate_far) for o, f in zip(own, far)]
    value_parts = [up(o, f, value_own, value_far) for o, f in zip(own, far)]

    conv_docs = jnp.concatenate([prev_docs[-2:], docs_plus], axis=0)
    part_docs = [
        lax.dynamic_slice_in_dim(conv_docs, i * part_rows, part_rows + 2, 0) for i in part_index
    ]

    def conv_parts(parts, taps):
        tails = [p[-2:] for p in parts]
        last = tails[0]
        for d in range(1, n_tp):
            last = jnp.where(part_index[d] == n_tp - 1, tails[d], last)
        prev = shifted(last, "sp", 1)
        result = []
        for d in range(n_tp):
            halo = jnp.where(part_index[d] == 0, prev, tails[(d + 1) % n_tp])
            result.append(
                convolve(jnp.concatenate([halo, parts[d]], axis=0), part_docs[d], taps)
            )
        return result

    gate_conv = conv_parts(gate_parts, conv_gate)
    value_conv = conv_parts(value_parts, conv_value)
    hidden = [
        (jax.nn.silu(g) * v).astype(jnp.bfloat16) for g, v in zip(gate_conv, value_conv)
    ]

    def down(units, w_t):
        return lax.dot_general(
            units, w_t, (((1,), (1,)), ((), ())), preferred_element_type=jnp.float32
        )

    own_units = [jnp.where(core == 0, h[:, :inner], h[:, inner:]) for h in hidden]
    far_units = [jnp.where(core == 0, h[:, inner:], h[:, :inner]) for h in hidden]

    def down_sums(w_own):
        w_far = core_swap(w_own)
        came = []
        for d in range(1, n_tp):
            sent = (down(own_units[d], w_own) + down(far_units[d], w_far)).astype(
                jnp.bfloat16
            )
            came.append(turned(sent, "tp", -d))
        kept = down(own_units[0], w_own) + down(far_units[0], w_far)
        for t in came:
            kept = kept + t.astype(jnp.float32)
        return kept

    odd_sum = down_sums(down_odd)
    even_sum = down_sums(down_even)
    sums = (even_sum, odd_sum)
    return finish(mid, sums, depth)


def solution(mesh):
    return jax.shard_map(
        per_device,
        mesh=mesh,
        in_specs=(
            P("sp", "tp"),
            P("sp", "tp"),
            P("sp", "tp"),
            P("sp"),
            P("tp"),
            P(("sp", "tp"), None),
            P("tp", None),
            P(),
            P("sp", "tp"),
            P("sp", "tp"),
            P(None, "tp"),
            P(None, "tp"),
            P("tp", "sp"),
        ),
        out_specs=P(("sp", "tp"), None),
        check_vma=False,
    )
```
